512 devices in a mesh: sp: 64 (over z, y), dp: 8 (over x, core).
Axes of the slice: x: 4, y: 4, z: 16, core: 2. Of those that a mesh axis runs over, the one named last changes fastest.
Arguments:
- tokens: bfloat16 [16384, 2048], P('sp'), may hold values from -16 to 16
- w_carry: bfloat16 [2048, 1024], P(None, 'dp'), may hold values from -0.125 to 0.125
- w_gate: bfloat16 [2048, 1024], P(None, 'dp'), may hold values from -8 to 8
- mix_weight: bfloat16 [8, 128, 128], P('dp'), may hold values from -0.5 to 0.5
- mix_bias: float32 [8, 128], P('dp'), may hold values from 0.1 to 1.9
- ln_gain: float32 [1024], P('dp'), may hold values from 0.1 to 1.9
- ln_shift: float32 [1024], P('dp'), may hold values from -3 to 3
- cotangent: bfloat16 [16384, 1024], P('sp', 'dp'), may hold values from -6 to 6
Outputs:
- grad_input: bfloat16 [16384, 2048], P('sp')
- grad_carry: float32 [2048, 1024], P('sp', 'dp')
- grad_gate: float32 [2048, 1024], P('sp', 'dp')
- grad_mix: float32 [8, 128, 128], P('dp')
- grad_bias: float32 [8, 128], P('dp')
- grad_gain: float32 [1024], P('dp')
- grad_shift: float32 [1024], P('dp')
The draws below stay inside these ranges and needn't reach their ends.
All inputs are finite; a program needn't handle non-finite values.
Results may differ from the reference program's by a relative error of at most 0.017.
Values may be sent and summed in bfloat16 or wider, within the bound.
No kernel may reach another device: no remote copies, remote signals or barrier semaphores. Data moves between devices by JAX's collectives and lax.ppermute only.
A program may use at most 64 MiB of HBM per device.

```python
import math
import jax
import jax.numpy as jnp
from jax import lax

D = 2048
GROUPS = 8
GROUP_DIM = 128
SPAN = 128
SEGMENT = 64
TW = 1024
TOKENS = 16384
N_DP = 8


def draw_w_gate(key, part):
    key_spread = jax.random.fold_in(key, 11)
    key_entries = jax.random.fold_in(key, 23)
    column_pos = jnp.arange(TW).astype(jnp.float32) / (TW - 1)
    spread = jax.random.uniform(key_spread, (TW,), jnp.float32, 0.0, math.log(10.0))
    entries = jnp.clip(jax.random.normal(key_entries, (D, TW), jnp.float32), -6.0, 6.0)
    col_scale = 0.3 * jnp.exp(column_pos * math.log(3.0) + spread) * D ** (-0.5)
    return (entries * col_scale[None, :]).astype(jnp.bfloat16)


def spiked(values, rng, source, target, shards_of, factor):
    owner, partner = [(jnp.arange(values.shape[position]) // (values.shape[position] // shards_of)).reshape([-1 if axis == position else 1 for axis in range(values.ndim)]) for position in (source, target)]
    chosen = jax.random.permutation(rng, shards_of)[partner]
    strong = (owner == chosen) | (owner == (partner + shards_of // 2) % shards_of)
    return jnp.where(strong, factor * values, values)


def shard_levels(stream_key, extent, split, low, largest):
    level, own = 1.0, jax.random.fold_in(stream_key, 6)
    for position, shards_of in split:
        heights = jnp.exp(jax.random.uniform(jax.random.fold_in(own, position), (shards_of,), jnp.float32, low / len(split), largest / len(split)))
        level = level * jnp.repeat(heights, extent[position] // shards_of).reshape([-1 if axis == position else 1 for axis in range(len(extent))])
    return level


def scatter_about(rng, dims, width, most, shards=(), held_as=jnp.bfloat16):
    array = jax.random.normal(rng, dims, jnp.float32) * width
    if len(shards) > 0:
        array = shard_levels(rng, dims, shards, -0.22, 0.18) * array
    return jnp.clip(array, min=-most, max=most).astype(held_as)


def bell_draw_with(rng, dims, width, bound, shards, heavy, held_as=jnp.bfloat16):
    values = width * jax.random.normal(rng, dims, jnp.float32)
    if shards:
        values = values * shard_levels(rng, dims, shards, -0.22, 0.18)
    return jnp.clip(spiked(values, jax.random.fold_in(rng, 3), *heavy), -bound, bound).astype(held_as)


def setup_inputs(seed: int = 0) -> dict:
    key_list = jax.random.split(jax.random.key(seed), 9)
    return {
        "tokens": bell_draw_with(key_list[0], (TOKENS, D), 1.0, 16.0, ((0, 64),), (0, 1, 64, 4.0)),
        "w_carry": scatter_about(key_list[1], (D, TW), D ** -0.5, 0.125, ((1, 8),)),
        "w_gate": draw_w_gate(jax.random.fold_in(key_list[8], 71), 0),
        "mix_weight": scatter_about(key_list[3], (GROUPS, SPAN, SPAN), SPAN ** -0.5, 0.5, ((0, 8),)),
        "mix_bias": jnp.clip(1.0 + 0.18 * jax.random.normal(key_list[4], (GROUPS, SPAN), jnp.float32), 0.1, 1.9),
        "ln_gain": jnp.clip(1.0 + 0.18 * jax.random.normal(key_list[5], (TW,), jnp.float32), 0.1, 1.9),
        "ln_shift": scatter_about(key_list[6], (TW,), 0.5, 3.0, ((0, 8),), jnp.float32),
        "cotangent": scatter_about(key_list[7], (TOKENS, TW), 1.0, 6.0, ((0, 64), (1, 8))),
    }


sqrt_half = 0.7071067811865476
density = 0.3989422804014327
epsilon = 1e-06

def gelu_slope(inputs):
    return 0.5 * (1.0 + lax.erf(inputs * sqrt_half)) + inputs * jnp.exp(-0.5 * inputs * inputs) * density

def block_visible():
    segment = jnp.arange(SPAN) // SEGMENT
    return (segment[:, None] >= segment[None, :]).astype(jnp.float32)

def reference(tokens, w_carry, w_gate, mix_weight, mix_bias, ln_gain, ln_shift, cotangent):
    highest = lax.Precision.HIGHEST
    carry_pre = jnp.dot(tokens, w_carry, preferred_element_type=jnp.float32).astype(jnp.bfloat16)
    gate_pre = jnp.dot(tokens, w_gate, preferred_element_type=jnp.float32).astype(jnp.bfloat16)
    carry_wide = carry_pre.astype(jnp.float32)
    gate_wide = gate_pre.astype(jnp.float32)
    carried = jax.nn.gelu(carry_wide, approximate=False)
    gate_act = jax.nn.gelu(gate_wide, approximate=False)
    average = lax.optimization_barrier(jnp.mean(gate_act, axis=-1, keepdims=True))
    centered = gate_act - average
    rstd = lax.rsqrt(lax.optimization_barrier(jnp.mean(centered * centered, axis=-1, keepdims=True)) + epsilon)
    normed = centered * rstd
    gated_in = normed * ln_gain[None, :] + ln_shift[None, :]
    blocks = tokens.shape[0] // SPAN
    weights = mix_weight.astype(jnp.float32) * block_visible()[None]
    gated_four = gated_in.reshape(blocks, SPAN, GROUPS, GROUP_DIM)
    spatial = jnp.einsum('gts,nsgc->ntgc', weights, gated_four, precision=highest)
    spatial = spatial + mix_bias.T[None, :, :, None]
    spatial = spatial.reshape(tokens.shape[0], TW)
    upstream = cotangent.astype(jnp.float32)
    d_carry_pre = (upstream * spatial * gelu_slope(carry_wide)).astype(jnp.bfloat16)
    d_spatial = (upstream * carried).reshape(blocks, SPAN, GROUPS, GROUP_DIM)
    d_gated_four = jnp.einsum('gts,ntgc->nsgc', weights, d_spatial, precision=highest)
    d_gated_in = d_gated_four.reshape(tokens.shape[0], TW)
    d_normed = d_gated_in * ln_gain[None, :]
    d_gate_act = rstd * (d_normed - lax.optimization_barrier(jnp.mean(d_normed, axis=-1, keepdims=True)) - normed * lax.optimization_barrier(jnp.mean(d_normed * normed, axis=-1, keepdims=True)))
    d_gate_pre = (d_gate_act * gelu_slope(gate_wide)).astype(jnp.bfloat16)
    block_width = TW // N_DP
    summed = jnp.zeros((tokens.shape[0], D), jnp.float32)
    for column_block in range(N_DP):
        lower = column_block * block_width
        upper = lower + block_width
        partial_value = jnp.dot(d_carry_pre[:, lower:upper], w_carry[:, lower:upper].T, preferred_element_type=jnp.float32)
        partial_value = partial_value + jnp.dot(d_gate_pre[:, lower:upper], w_gate[:, lower:upper].T, preferred_element_type=jnp.float32)
        rounded = lax.optimization_barrier(partial_value.astype(jnp.bfloat16))
        summed = summed + rounded.astype(jnp.float32)
    grad_input = summed.astype(jnp.bfloat16)
    loss_scale = 1.0 / jnp.sqrt(jnp.float32(tokens.shape[0]))
    grad_carry = jnp.dot(tokens.T, d_carry_pre, preferred_element_type=jnp.float32) * loss_scale
    grad_gate = jnp.dot(tokens.T, d_gate_pre, preferred_element_type=jnp.float32) * loss_scale
    grad_mix = jnp.einsum('ntgc,nsgc->gts', d_spatial, gated_four, precision=highest) * block_visible()[None] * loss_scale
    grad_bias = lax.optimization_barrier(jnp.sum(d_spatial, axis=(0, 3))).T * loss_scale
    grad_gain = lax.optimization_barrier(jnp.sum(d_gated_in * normed, axis=0)) * loss_scale
    grad_shift = lax.optimization_barrier(jnp.sum(d_gated_in, axis=0)) * loss_scale
    return (grad_input, grad_carry, grad_gate, grad_mix, grad_bias, grad_gain, grad_shift)
```

```python
import math

import jax
import jax.numpy as jnp
from jax import lax
from jax.sharding import Mesh
from jax.sharding import PartitionSpec as P

GROUP_DIM = 128
SPAN = 128
SEGMENT = 64
SP = ("z", "y")
DP = ("x", "c")
SWAP = ((0, 1), (1, 0))

sqrt_half = 0.7071067811865476
density = 0.3989422804014327
epsilon = 1e-06
bf16 = jnp.bfloat16
f32 = jnp.float32


def exchange(tiles, axes):
    return lax.all_to_all(tiles, axes, split_axis=0, concat_axis=0, tiled=True)


def to_all(value, axes):
    return exchange(jnp.broadcast_to(value, (lax.axis_size(axes), *value.shape)), axes)


def gelu_slope(inputs):
    return (
        0.5 * (1.0 + lax.erf(inputs * sqrt_half))
        + inputs * jnp.exp(-0.5 * inputs * inputs) * density
    )


def block_visible():
    segment = jnp.arange(SPAN) // SEGMENT
    return (segment[:, None] >= segment[None, :]).astype(f32)


def two_parts(value):
    high = lax.reduce_precision(value, 8, 7)
    return high.astype(bf16), (value - high).astype(bf16)


def shards(tokens, w_carry, w_gate, mix_weight, mix_bias, ln_gain, ln_shift, cotangent):
    highest = lax.Precision.HIGHEST
    rows, model = tokens.shape
    owned = w_carry.shape[1]
    n_dp = lax.axis_size(DP)
    n_x, n_y, n_z = lax.axis_size("x"), lax.axis_size("y"), lax.axis_size("z")
    channels = owned * n_dp
    blocks = rows // SPAN
    loss_scale = 1.0 / math.sqrt(rows * n_y * n_z)

    carry_pre = jnp.dot(tokens, w_carry, preferred_element_type=f32).astype(bf16)
    gate_pre = jnp.dot(tokens, w_gate, preferred_element_type=f32).astype(bf16)
    carry_wide = carry_pre.astype(f32)
    gate_wide = gate_pre.astype(f32)
    carried = jax.nn.gelu(carry_wide, approximate=False)
    gate_act = jax.nn.gelu(gate_wide, approximate=False)
    upstream = cotangent.astype(f32)
    weights = mix_weight[0].astype(f32) * block_visible()
    d_spatial = upstream * carried
    d_spatial_b = d_spatial.reshape(blocks, SPAN, owned)
    d_gated_in = jnp.einsum("ts,ntc->nsc", weights, d_spatial_b, precision=highest)
    d_gated_in = d_gated_in.reshape(rows, owned)
    d_normed = d_gated_in * ln_gain[None, :]

    mean_a = jnp.mean(gate_act, axis=1)
    mean_d = jnp.mean(d_normed, axis=1)
    off_a = gate_act - mean_a[:, None]
    square = jnp.sum(off_a * off_a, axis=1)
    cross = jnp.sum(off_a * (d_normed - mean_d[:, None]), axis=1)
    stats = jnp.stack([mean_a, mean_d, square, cross]).reshape(4 * blocks, SPAN)
    stats = to_all(stats, DP).reshape(n_dp, 4, rows)
    average = jnp.mean(stats[:, 0], axis=0)
    d_average = jnp.mean(stats[:, 1], axis=0)
    shift_a = stats[:, 0] - average
    shift_d = stats[:, 1] - d_average
    square = jnp.sum(stats[:, 2], axis=0) + owned * jnp.sum(shift_a * shift_a, axis=0)
    cross = jnp.sum(stats[:, 3], axis=0) + owned * jnp.sum(shift_a * shift_d, axis=0)
    rstd = lax.rsqrt(square / channels + epsilon)
    slope_in = rstd * cross / channels

    normed = (gate_act - average[:, None]) * rstd[:, None]
    gated_in = normed * ln_gain[None, :] + ln_shift[None, :]
    gated_b = gated_in.reshape(blocks, SPAN, owned)
    spatial = jnp.einsum("ts,nsc->ntc", weights, gated_b, precision=highest)
    spatial = (spatial + mix_bias[0][None, :, None]).reshape(rows, owned)
    d_carry_pre = (upstream * spatial * gelu_slope(carry_wide)).astype(bf16)
    d_gate_act = rstd[:, None] * (
        d_normed - d_average[:, None] - normed * slope_in[:, None]
    )
    d_gate_pre = (d_gate_act * gelu_slope(gate_wide)).astype(bf16)
    d_pre = jnp.concatenate([d_carry_pre, d_gate_pre], axis=1)

    mix_term = jnp.einsum("ntc,nsc->ts", d_spatial_b, gated_b, precision=highest)
    bias_term = jnp.sum(d_spatial_b, axis=(0, 2))
    gain_term = jnp.sum(d_gated_in * normed, axis=0)
    shift_term = jnp.sum(d_gated_in, axis=0)
    corner = mix_term[:SEGMENT, :SEGMENT]
    seen = jnp.concatenate(
        [
            mix_term[SEGMENT:],
            jnp.concatenate([corner[: SEGMENT // 2], corner[SEGMENT // 2 :]], axis=1),
        ]
    )
    part = seen.shape[0] // n_y
    lines = jnp.stack([bias_term, gain_term, shift_term, jnp.zeros_like(bias_term)])
    small = jnp.concatenate(
        [seen.reshape(n_y, part, SPAN), lines[:, None], jnp.zeros((n_y, 7, SPAN), f32)],
        axis=1,
    )
    small = jnp.concatenate(two_parts(small), axis=2)
    grads = jnp.einsum("tr,tc->rc", tokens, d_pre, preferred_element_type=f32)
    piece = model // (n_y * n_z)
    grads = grads.astype(bf16).reshape(n_z, n_y, piece, 2 * owned)
    grads = grads.transpose(1, 0, 2, 3).reshape(n_y, n_z * piece, 2 * owned)
    arrived = exchange(jnp.concatenate([grads, small], axis=1), "y").astype(f32)
    arrived = jnp.sum(arrived, axis=0)
    grads = arrived[: n_z * piece].astype(bf16).reshape(n_z, piece, 2 * owned)
    small = arrived[n_z * piece :]
    small = small[:, :SPAN] + small[:, SPAN:]
    line_high, line_low = two_parts(small[part : part + 1])
    half = part // 2
    small = jnp.concatenate(
        [
            jnp.concatenate([small[:half], small[half:part]], axis=1).astype(bf16),
            jnp.concatenate([line_high, line_low], axis=1),
            jnp.zeros((3, 2 * SPAN), bf16),
        ]
    )
    small = jnp.broadcast_to(small, (n_z, *small.shape))
    arrived = exchange(jnp.concatenate([grads, small], axis=1), "z").astype(f32)
    arrived = jnp.sum(arrived, axis=0) * loss_scale
    grad_carry = arrived[:piece, :owned]
    grad_gate = arrived[:piece, owned:]
    small = arrived[piece:]
    line = small[half : half + 1]
    small = jnp.concatenate(
        [
            small[:half, :SPAN],
            small[:half, SPAN:],
            line[:, :SPAN] + line[:, SPAN:],
            jnp.zeros((7, SPAN), f32),
        ]
    )
    small = to_all(small, "y")
    lines = small[:, part]
    seen = small[:, :part].reshape(n_y * part, SPAN)
    corner = seen[SEGMENT:]
    corner = jnp.concatenate([corner[:, :SEGMENT], corner[:, SEGMENT:]])
    corner = jnp.concatenate([corner, jnp.zeros_like(corner)], axis=1)
    grad_mix = jnp.concatenate([corner, seen[:SEGMENT]])[None]
    grad_bias = lines[:1]
    grad_gain = lines[1]
    grad_shift = lines[2]

    partial = jnp.einsum("tc,dc->td", d_carry_pre, w_carry, preferred_element_type=f32)
    partial = partial + jnp.einsum("tc,dc->td", d_gate_pre, w_gate, preferred_element_type=f32)
    partial = partial.astype(bf16)
    core = lax.axis_index("c")
    low, high = partial[:, : model // 2], partial[:, model // 2 :]
    mine = jnp.where(core == 0, low, high)
    theirs = lax.ppermute(jnp.where(core == 0, high, low), "c", SWAP)
    pair = (mine.astype(f32) + theirs.astype(f32)).astype(bf16)
    pair = exchange(pair.reshape(n_x, rows // n_x, model // 2), "x")
    final = jnp.sum(pair.astype(f32), axis=0).astype(bf16)
    final = to_all(final, DP).reshape(n_x, 2, rows // n_x, model // 2)
    grad_input = final.transpose(0, 2, 1, 3).reshape(rows, model)
    return grad_input, grad_carry, grad_gate, grad_mix, grad_bias, grad_gain, grad_shift


def solution(mesh):
    finer = Mesh(mesh.devices.reshape(16, 4, 4, 2), ("z", "y", "x", "c"))
    placed = (
        P(SP, None),
        P(None, DP),
        P(None, DP),
        P(DP, None, None),
        P(DP, None),
        P(DP),
        P(DP),
        P(SP, DP),
    )
    return jax.shard_map(
        shards,
        mesh=finer,
        in_specs=placed,
        out_specs=(
            P(SP, None),
            P(SP, DP),
            P(SP, DP),
            P(DP, None, None),
            P(DP, None),
            P(DP),
            P(DP),
        ),
        check_vma=False,
    )
```

```python
import math

import jax
import jax.numpy as jnp
from jax import lax
from jax.experimental import pallas as pl
from jax.experimental.pallas import tpu as pltpu
from jax.sharding import Mesh
from jax.sharding import PartitionSpec as P

SPAN = 128
SEGMENT = 64
SP = ("z", "y")
DP = ("x", "c")
SWAP = ((0, 1), (1, 0))

sqrt_half = 0.7071067811865476
density = 0.3989422804014327
epsilon = 1e-06
bf16 = jnp.bfloat16
f32 = jnp.float32
highest = lax.Precision.HIGHEST


def exchange(tiles, axes):
    return lax.all_to_all(tiles, axes, split_axis=0, concat_axis=0, tiled=True)


def ahead(value, axis, k):
    n = lax.axis_size(axis)
    return lax.ppermute(value, axis, [(i, (i + k) % n) for i in range(n)])


def call(body, outs, *args, flops=1, scalars=0, scratch=(), moved=1):
    smem = pl.BlockSpec(memory_space=pltpu.SMEM)
    vmem = pl.BlockSpec(memory_space=pltpu.VMEM)
    return pl.pallas_call(
        body,
        out_shape=[jax.ShapeDtypeStruct(s, d) for s, d in outs],
        in_specs=[smem] * scalars + [vmem] * (len(args) - scalars),
        out_specs=[vmem] * len(outs),
        scratch_shapes=list(scratch),
        cost_estimate=pl.CostEstimate(flops=flops, bytes_accessed=moved, transcendentals=0),
    )(*args)


def dot(a, b, precision=None):
    return lax.dot_general(
        a, b, (((1,), (0,)), ((), ())), precision=precision, preferred_element_type=f32
    )


def dot_t(a, b, precision=None):
    return lax.dot_general(
        a, b, (((1,), (1,)), ((), ())), precision=precision, preferred_element_type=f32
    )


def visible(weights):
    t = lax.broadcasted_iota(jnp.int32, (SPAN, SPAN), 0)
    s = lax.broadcasted_iota(jnp.int32, (SPAN, SPAN), 1)
    return jnp.where(t // SEGMENT >= s // SEGMENT, weights.astype(f32), 0.0)


def gelu(v):
    return 0.5 * v * (1.0 + lax.erf(v * sqrt_half))


def gelu_slope(v):
    return 0.5 * (1.0 + lax.erf(v * sqrt_half)) + v * jnp.exp(-0.5 * v * v) * density


def local_part(tok, wc, wg, mix, gain, cot, carry, gate, act, ds, dg, stats, acc_c, acc_g):
    step = pl.program_id(0)

    @pl.when(step == 0)
    def _():
        acc_c[...] = jnp.zeros_like(acc_c)
        acc_g[...] = jnp.zeros_like(acc_g)

    acc_c[...] += dot(tok[...], wc[...])
    acc_g[...] += dot(tok[...], wg[...])

    @pl.when(step == pl.num_programs(0) - 1)
    def _():
        carry[...] = acc_c[...].astype(bf16)
        gate[...] = acc_g[...].astype(bf16)
        owned = wc.shape[1]
        weights = visible(mix[0])
        ones = jnp.ones((8, owned), f32)
        rows = []
        for b in range(tok.shape[0] // SPAN):
            here = pl.ds(b * SPAN, SPAN)
            a = gelu(gate[here, :].astype(f32))
            act[here, :] = a
            d = cot[here, :].astype(f32) * gelu(carry[here, :].astype(f32))
            ds[here, :] = d
            back = lax.dot_general(
                weights, d, (((0,), (0,)), ((), ())), precision=highest, preferred_element_type=f32
            )
            dg[here, :] = back
            n = back * gain[...]
            off_a = a - jnp.mean(a, axis=1, keepdims=True)
            off_n = n - jnp.mean(n, axis=1, keepdims=True)
            rows.append(
                (
                    dot_t(ones, a, highest)[:1] / owned,
                    dot_t(ones, n, highest)[:1] / owned,
                    dot_t(ones, off_a * off_a, highest)[:1],
                    dot_t(ones, off_a * off_n, highest)[:1],
                )
            )
        table = jnp.concatenate([r[k] for k in range(4) for r in rows], axis=0)
        for j in range(stats.shape[0]):
            stats[j] = table


def turned(tok, carry, gate, cot, turned_tok, slope_c, slope_g):
    n_y = turned_tok.shape[0]
    piece = 32
    wide = 8 * piece * n_y // 2
    for at in range(0, tok.shape[1], wide):
        block = jnp.transpose(tok[:, at : at + wide])
        for q in range(wide // piece):
            k = at // piece + q
            turned_tok[k % n_y, pl.ds(k // n_y * piece, piece), :] = block[q * piece : q * piece + piece]
    slope_c[...] = cot[...].astype(f32) * gelu_slope(carry[...].astype(f32))
    slope_g[...] = gelu_slope(gate[...].astype(f32))


def normal_part(
    stats, act, ds, dg, slope_c, slope_g, mix, bias, gain, shift, tok_t, sent, d_pre
):
    n, owned = stats.shape[0], act.shape[1]
    st = stats[...]
    mean = jnp.sum(st, axis=0) / n
    dev = st[:, 0:4] - mean[None, 0:4]
    dev_a, dev_d = dev[:, 0:2], dev[:, 2:4]
    square = n * mean[4:6] + owned * jnp.sum(dev_a * dev_a, axis=0)
    cross = n * mean[6:8] + owned * jnp.sum(dev_a * dev_d, axis=0)
    rstd = lax.rsqrt(square / (n * owned) + epsilon)
    table = jnp.concatenate([mean[0:4], rstd, rstd * cross / (n * owned)], axis=0)
    table = jnp.transpose(table)
    weights = visible(mix[0])
    bias_col = jnp.transpose(jnp.broadcast_to(bias[...], (8, SPAN)))[:, 0:1]
    mix_sum = jnp.zeros((SPAN, SPAN), f32)
    gain_sum = jnp.zeros((1, owned), f32)
    shift_sum = jnp.zeros((1, owned), f32)
    ds_sum = jnp.zeros((SPAN, owned), f32)
    for b in range(2):
        here = pl.ds(b * SPAN, SPAN)
        inv = table[:, 4 + b : 5 + b]
        normed = (act[here, :] - table[:, b : b + 1]) * inv
        gated = normed * gain[...] + shift[...]
        spatial = dot(weights, gated, highest) + bias_col
        d_pre[here, 0:owned] = (slope_c[here, :] * spatial).astype(bf16)
        back = dg[here, :]
        d_act = inv * (
            back * gain[...] - table[:, 2 + b : 3 + b] - normed * table[:, 6 + b : 7 + b]
        )
        d_pre[here, owned:] = (d_act * slope_g[here, :]).astype(bf16)
        d = ds[here, :]
        mix_sum += dot_t(d, gated, highest)
        ds_sum += d
        gain_sum += jnp.sum(back * normed, axis=0, keepdims=True)
        shift_sum += jnp.sum(back, axis=0, keepdims=True)
    bias_sum = dot_t(jnp.ones((8, owned), f32), ds_sum, highest)[:1]
    lane = lax.broadcasted_iota(jnp.int32, (SEGMENT // 2, SPAN), 1)
    corner = jnp.where(
        lane < SEGMENT,
        mix_sum[: SEGMENT // 2],
        pltpu.roll(mix_sum[SEGMENT // 2 : SEGMENT], SEGMENT, 1),
    )
    seen = jnp.concatenate([mix_sum[SEGMENT:], corner], axis=0)
    row = lax.broadcasted_iota(jnp.int32, (8, SPAN), 0)
    lines = (bias_sum, gain_sum, shift_sum, jnp.zeros_like(bias_sum))
    grads_at = tok_t.shape[1]
    part = seen.shape[0] // sent.shape[0]
    for j in range(sent.shape[0]):
        line = jnp.where(row == 0, jnp.broadcast_to(lines[j], (8, SPAN)), 0.0)
        small = jnp.concatenate([seen[j * part : j * part + part], line], axis=0)
        high = small.astype(bf16)
        sent[j, grads_at:, 0:SPAN] = high
        sent[j, grads_at:, SPAN:] = (small - high.astype(f32)).astype(bf16)
    for j in range(sent.shape[0]):
        sent[j, 0:grads_at, :] = dot(tok_t[j], d_pre[...]).astype(bf16)


def summed_y(came, sent):
    n_z = sent.shape[0]
    piece = 32
    grads_at = n_z * piece
    total = came[0].astype(f32)
    for j in range(1, came.shape[0]):
        total = total + came[j].astype(f32)
    small = total[grads_at:, 0:SPAN] + total[grads_at:, SPAN:]
    row = lax.broadcasted_iota(jnp.int32, (8, SPAN), 0)
    line = jnp.broadcast_to(small[24:25], (8, SPAN))
    high = line.astype(bf16).astype(f32)
    line = jnp.where(row == 0, high, jnp.where(row == 1, line - high, 0.0))
    right = jnp.concatenate([small[16:24], line], axis=0)
    small = jnp.concatenate([small[0:16], right], axis=1).astype(bf16)
    for k in range(n_z):
        sent[k, 0:piece, :] = total[k * piece : k * piece + piece].astype(bf16)
        sent[k, piece:, :] = small


def summed_z(came, carry, gate, small, *, scale):
    total = came[0].astype(f32)
    for k in range(1, came.shape[0]):
        total = total + came[k].astype(f32)
    total = total * scale
    owned = carry.shape[1]
    carry[...] = total[0:32, 0:owned]
    gate[...] = total[0:32, owned:]
    row = lax.broadcasted_iota(jnp.int32, (8, SPAN), 0)
    line = jnp.broadcast_to(total[40:41, SPAN:] + total[41:42, SPAN:], (8, SPAN))
    line = jnp.where(row == 0, line, 0.0)
    part = jnp.concatenate([total[32:48, 0:SPAN], total[32:40, SPAN:], line], axis=0)
    for j in range(small.shape[0]):
        small[j] = part


def unpacked(small, mix, bias, gain, shift):
    lane = lax.broadcasted_iota(jnp.int32, (SEGMENT // 2, SPAN), 1)
    corner = jnp.concatenate([small[2, 16:24], small[3, 0:24]], axis=0)
    mix[0, 0 : SEGMENT // 2, :] = jnp.where(lane < SEGMENT, corner, 0.0)
    mix[0, SEGMENT // 2 : SEGMENT, :] = jnp.where(
        lane < SEGMENT, pltpu.roll(corner, SEGMENT, 1), 0.0
    )
    mix[0, 64:88, :] = small[0, 0:24]
    mix[0, 88:112, :] = small[1, 0:24]
    mix[0, 112:128, :] = small[2, 0:16]
    bias[...] = small[0, 24:25]
    gain[...] = small[1, 24:25]
    shift[...] = small[2, 24:25]


def theirs_part(at, d_pre, wc, wg, out):
    owned = wc.shape[1]
    half = out.shape[0]
    rows = d_pre[pl.ds(pl.multiple_of((1 - at[0]) * half, half), half), :]
    for n in range(0, out.shape[1], 512):
        here = pl.ds(n, 512)
        v = dot_t(rows[:, :owned], wc[here, :]) + dot_t(rows[:, owned:], wg[here, :])
        out[:, n : n + 512] = v.astype(bf16)


def pair_part(at, d_pre, wc, wg, came, own, one, two, three, held):
    owned = wc.shape[1]
    half, piece = held.shape[0], own.shape[0]
    rows = d_pre[pl.ds(pl.multiple_of(at[0] * half, half), half), :]
    for n in range(0, own.shape[1], 512):
        here = pl.ds(n, 512)
        v = dot_t(rows[:, :owned], wc[here, :]) + dot_t(rows[:, owned:], wg[here, :])
        held[:, n : n + 512] = v + came[:, n : n + 512].astype(f32)
    for k, out in enumerate((own, one, two, three)):
        first = pl.multiple_of(((at[1] + k) & 3) * piece, piece)
        out[...] = held[pl.ds(first, piece), :].astype(out.dtype)


def summed_x(own, one, two, three, out):
    total = own[...] + one[...].astype(f32) + two[...].astype(f32) + three[...].astype(f32)
    out[...] = total.astype(bf16)


def joined_x(at, own, one, two, three, out):
    piece = own.shape[0]
    for k, part in enumerate((own, one, two, three)):
        first = pl.multiple_of(((at[1] + 4 - k) & 3) * piece, piece)
        out[pl.ds(first, piece), :] = part[...]


def joined_pair(at, own, other, out):
    half = own.shape[0]
    out[pl.ds(pl.multiple_of(at[0] * half, half), half), :] = own[...]
    out[pl.ds(pl.multiple_of((1 - at[0]) * half, half), half), :] = other[...]


def shards(tokens, w_carry, w_gate, mix_weight, mix_bias, ln_gain, ln_shift, cotangent):
    rows, model = tokens.shape
    owned = w_carry.shape[1]
    n_dp = lax.axis_size(DP)
    n_x, n_y, n_z = lax.axis_size("x"), lax.axis_size("y"), lax.axis_size("z")
    loss_scale = 1.0 / math.sqrt(rows * n_y * n_z)
    gain, shift = ln_gain.reshape(1, owned), ln_shift.reshape(1, owned)
    at = jnp.stack([lax.axis_index("c"), lax.axis_index("x")]).astype(jnp.int32)

    steps = 4
    deep = model // steps
    whole = lambda shape: pl.BlockSpec(shape, lambda k: (0,) * len(shape))
    act_shape = jax.ShapeDtypeStruct((rows, owned), f32)
    carry, gate, act, ds, dg, stats = pl.pallas_call(
        local_part,
        grid=(steps,),
        in_specs=[
            pl.BlockSpec((rows, deep), lambda k: (0, k)),
            pl.BlockSpec((deep, owned), lambda k: (k, 0)),
            pl.BlockSpec((deep, owned), lambda k: (k, 0)),
            whole((1, SPAN, SPAN)),
            whole((1, owned)),
            whole((rows, owned)),
        ],
        out_specs=[whole((rows, owned))] * 5 + [whole((n_dp, 8, SPAN))],
        out_shape=[
            jax.ShapeDtypeStruct((rows, owned), bf16),
            jax.ShapeDtypeStruct((rows, owned), bf16),
            act_shape,
            act_shape,
            act_shape,
            jax.ShapeDtypeStruct((n_dp, 8, SPAN), f32),
        ],
        scratch_shapes=[pltpu.VMEM((rows, owned), f32)] * 2,
    )(tokens, w_carry, w_gate, mix_weight, gain, cotangent)

    stats = exchange(stats, DP)
    tok_t, slope_c, slope_g = call(
        turned,
        [((n_y, model // n_y, rows), bf16), ((rows, owned), f32), ((rows, owned), f32)],
        tokens, carry, gate, cotangent,
        flops=2 * 10**9, moved=2 * rows * model * 2,
    )
    sent, d_pre = call(
        normal_part,
        [((n_y, model // n_y + 32, 2 * owned), bf16), ((rows, 2 * owned), bf16)],
        stats, act, ds, dg, slope_c, slope_g, mix_weight, mix_bias, gain, shift, tok_t,
        flops=10**9, moved=2 * rows * model * 2,
    )

    with jax.named_scope("sum_y"):
        came = exchange(sent, "y")
    (sent,) = call(summed_y, [((n_z, 48, 2 * owned), bf16)], came, flops=10**9, moved=2 * came.size)
    with jax.named_scope("sum_z"):
        came = exchange(sent, "z")
    scaled = lambda *refs: summed_z(*refs, scale=loss_scale)
    piece = model // (n_y * n_z)
    grad_carry, grad_gate, small = call(
        scaled,
        [((piece, owned), f32), ((piece, owned), f32), ((n_y, 32, SPAN), f32)],
        came, flops=10**9, moved=2 * came.size,
    )
    with jax.named_scope("share_y"):
        small = exchange(small, "y")
    grad_mix, grad_bias, grad_gain, grad_shift = call(
        unpacked,
        [((1, SPAN, SPAN), f32), ((1, SPAN), f32), ((1, owned), f32), ((1, owned), f32)],
        small, flops=10**8, moved=4 * small.size,
    )

    half = rows // 2
    part = half // n_x
    (theirs,) = call(
        theirs_part, [((half, model), bf16)], at, d_pre, w_carry, w_gate,
        scalars=1, flops=10**9, moved=4 * half * model,
    )
    with jax.named_scope("pair_sum"):
        theirs = lax.ppermute(theirs, "c", SWAP)
    own, one, two, three = call(
        pair_part,
        [((part, model), f32)] + [((part, model), bf16)] * 3,
        at, d_pre, w_carry, w_gate, theirs,
        scalars=1, flops=10**9, moved=8 * half * model,
        scratch=[pltpu.VMEM((half, model), f32)],
    )
    with jax.named_scope("sum_x"):
        came = [ahead(v, "x", k) for k, v in ((1, one), (2, two), (3, three))]
    (final,) = call(summed_x, [((part, model), bf16)], own, *came, flops=10**8, moved=4 * own.size)
    with jax.named_scope("share_x"):
        came = [ahead(final, "x", k) for k in (1, 2, 3)]
    (joined,) = call(
        joined_x, [((half, model), bf16)], at, final, *came,
        scalars=1, flops=10**8, moved=4 * half * model,
    )
    with jax.named_scope("share_pair"):
        other = lax.ppermute(joined, "c", SWAP)
    (grad_input,) = call(
        joined_pair, [((rows, model), bf16)], at, joined, other,
        scalars=1, flops=10**8, moved=4 * rows * model,
    )
    return (
        grad_input,
        grad_carry,
        grad_gate,
        grad_mix,
        grad_bias,
        grad_gain.reshape(owned),
        grad_shift.reshape(owned),
    )


def solution(mesh):
    finer = Mesh(mesh.devices.reshape(16, 4, 4, 2), ("z", "y", "x", "c"))
    placed = (
        P(SP, None),
        P(None, DP),
        P(None, DP),
        P(DP, None, None),
        P(DP, None),
        P(DP),
        P(DP),
        P(SP, DP),
    )
    return jax.shard_map(
        shards,
        mesh=finer,
        in_specs=placed,
        out_specs=(
            P(SP, None),
            P(SP, DP),
            P(SP, DP),
            P(DP, None, None),
            P(DP, None),
            P(DP),
            P(DP),
        ),
        check_vma=False,
    )
```
